32 devices in a mesh: grp: 2 (over y), sp: 4 (over z), tp: 4 (over x, core).
Axes of the slice: x: 2, y: 2, z: 4, core: 2. Of those that a mesh axis runs over, the one named last changes fastest.
Arguments:
- query_first: bfloat16 [1536, 512], P(('grp', 'sp'), 'tp'), parts along dimension 0, may hold values from -172 to 172
- key_first: bfloat16 [1536, 512], P(('grp', 'sp'), 'tp'), parts along dimension 0, may hold values from -7.8 to 7.8
- query_second: bfloat16 [1536, 1024], P(('grp', 'sp'), 'tp'), parts along dimension 0, may hold values from -172 to 172
- key_second: bfloat16 [1536, 1024], P(('grp', 'sp'), 'tp'), parts along dimension 0, may hold values from -7.8 to 7.8
- values: bfloat16 [1536, 2, 512], P(('grp', 'sp'), None, 'tp'), parts along dimension 0, may hold values from -6 to 6
- lambdas: float32 [2, 4], P(None, 'tp'), may hold values from 0.3 to 0.8
- residual: bfloat16 [1536, 2048], P(('grp', 'sp'), 'tp'), parts along dimension 0, may hold values from -130 to 130
- norm_gain: bfloat16 [2048], P('tp'), may hold values from 0.099609375 to 1.8984375
- out_weight: bfloat16 [2, 512, 2048], P(None, 'tp'), may hold values from -0.1875 to 0.1875
- gate_weight: bfloat16 [2048, 5632], P('sp', 'tp'), may hold values from -0.125 to 0.125
- up_weight: bfloat16 [2048, 5632], P('sp', 'tp'), may hold values from -0.125 to 0.125
- down_weight: bfloat16 [5632, 2048], P('tp', 'sp'), may hold values from -0.078125 to 0.078125
Outputs:
- layer_out: bfloat16 [1536, 2048], P(('grp', 'sp'), 'tp'), parts along dimension 0
The draws below stay inside these ranges and needn't reach their ends.
There are 2 independent parts, one for each index of `grp`. The reference program is written for one: setup_inputs(seed, part) draws one part's arguments, and reference() takes and returns one part's arrays. A program takes and returns all parts, laid end to end along the dimension named above; an argument that names none is the same for every part. Nothing has to cross between parts.
All inputs are finite; a program needn't handle non-finite values.
Results may differ from the reference program's by a relative error of at most 0.0065.
Values may be sent and summed in bfloat16 or wider, within the bound.
A program may use at most 128 MiB of HBM per device.

```python
import jax
import jax.numpy as jnp
from jax import lax

D = 2048
FF = 5632
HEADS = 4
DKA = 64
DKB = 128
DV = 128
SEQ = 768


def paired_draw(key, salt, key_width):
    base = jax.random.fold_in(key, salt)
    key_draw = jax.random.normal(jax.random.fold_in(base, 1), (SEQ, HEADS * 2 * key_width), jnp.float32)
    query_draw = jax.random.normal(jax.random.fold_in(base, 2), (SEQ, HEADS * 2 * key_width), jnp.float32)
    keys_out = 1.3 * jnp.clip(key_draw, -6.0, 6.0)
    queries_out = 1.3 * jnp.clip(query_draw, -6.0, 6.0)
    return (queries_out, keys_out)


def draw_query_first(key, part):
    return paired_draw(key, 11, DKA)[0].astype(jnp.bfloat16)


def draw_key_first(key, part):
    return paired_draw(key, 11, DKA)[1].astype(jnp.bfloat16)


def draw_query_second(key, part):
    return paired_draw(key, 23, DKB)[0].astype(jnp.bfloat16)


def draw_key_second(key, part):
    return paired_draw(key, 23, DKB)[1].astype(jnp.bfloat16)


def draw_residual(key, part):
    base = jax.random.fold_in(key, 37)
    entries = jnp.clip(jax.random.normal(jax.random.fold_in(base, 1), (SEQ, D), jnp.float32), -6.0, 6.0)
    jitter = jnp.clip(jax.random.normal(jax.random.fold_in(base, 2), (1, D), jnp.float32), -2.0, 2.0)
    column = 0.3 * 10.0 ** (jnp.arange(D, dtype=jnp.float32)[None, :] / D + 0.1 * jitter)
    row_scale = 0.3 * 10.0 ** jax.random.uniform(jax.random.fold_in(base, 3), (SEQ, 1), jnp.float32)
    result = entries * column * row_scale
    return result.astype(jnp.bfloat16)


def block_scale(rng, dims, pieces, low, top_value):
    def one(axis_at, parts):
        heights = jax.random.uniform(jax.random.fold_in(jax.random.fold_in(rng, 6), axis_at), (parts,), jnp.float32, low / len(pieces), top_value / len(pieces))
        return jnp.repeat(jnp.exp(heights), dims[axis_at] // parts).reshape((-1,) + (1,) * (len(dims) - axis_at - 1))

    factor_of = one(*pieces[0])
    for cut in pieces[1:]:
        factor_of = factor_of * one(*cut)
    return factor_of


def bell_draw(rng, shape, spread, reach, pieces=(), held_as=jnp.bfloat16):
    values = jax.random.normal(rng, shape, jnp.float32) * spread
    if len(pieces) > 0:
        values = block_scale(rng, shape, pieces, -0.22, 0.18) * values
    return jnp.clip(values, min=-reach, max=reach).astype(held_as)


def setup_inputs(seed: int = 0, part: int = 0) -> dict:
    seeds = jax.random.split(jax.random.key(seed), 13)
    own_keys = jax.random.split(jax.random.fold_in(seeds[12], part), 13)
    query_first = draw_query_first(jax.random.fold_in(jax.random.fold_in(seeds[12], part), 71), part)
    key_first = draw_key_first(jax.random.fold_in(jax.random.fold_in(seeds[12], part), 71), part)
    query_second = draw_query_second(jax.random.fold_in(jax.random.fold_in(seeds[12], part), 71), part)
    key_second = draw_key_second(jax.random.fold_in(jax.random.fold_in(seeds[12], part), 71), part)
    values = bell_draw(own_keys[4], (SEQ, 2, HEADS * DV), 1.0, 6.0, ((0, 4), (2, 4)))
    lambdas = jnp.clip(0.3 + 0.5 * jax.random.uniform(seeds[5], (2, HEADS), jnp.float32) ** block_scale(seeds[5], (2, HEADS), ((1, 4),), -0.2, 0.2), 0.3, 0.8)
    residual = draw_residual(jax.random.fold_in(jax.random.fold_in(seeds[12], part), 71), part)
    norm_gain = jnp.clip(1.0 + 0.18 * jax.random.normal(seeds[7], (D,), jnp.float32), 0.099609375, 1.8984375).astype(jnp.bfloat16)
    out_weight = bell_draw(seeds[8], (2, HEADS * DV, D), (2 * HEADS * DV) ** -0.5, 0.1875, ((1, 4),))
    gate_weight = bell_draw(seeds[9], (D, FF), D ** -0.5, 0.125, ((0, 4), (1, 4)))
    up_weight = bell_draw(seeds[10], (D, FF), D ** -0.5, 0.125, ((0, 4), (1, 4)))
    down_weight = bell_draw(seeds[11], (FF, D), FF ** -0.5, 0.078125, ((0, 4), (1, 4)))
    return dict(query_first=query_first, key_first=key_first, query_second=query_second, key_second=key_second, values=values, lambdas=lambdas, residual=residual, norm_gain=norm_gain, out_weight=out_weight, gate_weight=gate_weight, up_weight=up_weight, down_weight=down_weight)


def one_head(query_rows, key_rows, value_rows, lam_value, key_width):
    block_rows = 512 if SEQ % 512 == 0 else SEQ
    blocks = SEQ // block_rows
    query_blocks = query_rows.reshape(blocks, block_rows, 2, key_width)
    starts = jnp.arange(blocks, dtype=jnp.int32) * block_rows
    key_pos = jnp.arange(SEQ, dtype=jnp.int32)[None, :]
    key_f32 = key_rows.astype(jnp.float32)
    value_f32 = value_rows.astype(jnp.float32)

    def per_block(inputs):
        query_block, offset = inputs
        query_pos = offset + jnp.arange(block_rows, dtype=jnp.int32)[:, None]
        allowed = key_pos <= query_pos
        scores = jnp.einsum('qmd,kmd->mqk', query_block.astype(jnp.float32), key_f32) * key_width ** (-0.5)
        scores = jnp.where(allowed, scores, -1e+30)
        peak = lax.optimization_barrier(jnp.max(scores, axis=-1, keepdims=True))
        weights = jnp.where(allowed, jnp.exp(scores - peak), 0.0)
        totals = lax.optimization_barrier(jnp.sum(weights, axis=-1, keepdims=True))
        rounded = weights.astype(jnp.bfloat16).astype(jnp.float32)
        map_out = jnp.einsum('mqk,ke->mqe', rounded, value_f32) / totals
        differ = map_out[0] - lam_value * map_out[1]
        scale = lax.rsqrt(lax.optimization_barrier(jnp.mean(differ * differ, axis=-1, keepdims=True)) + 1e-06)
        return (0.8 * differ * scale).astype(jnp.bfloat16)
    result = lax.map(per_block, (query_blocks, starts))
    return result.reshape(SEQ, DV)

def reference(query_first, key_first, query_second, key_second, values, lambdas, residual, norm_gain, out_weight, gate_weight, up_weight, down_weight):
    mixed = jnp.zeros((SEQ, D), jnp.float32)
    groups = ((query_first, key_first, DKA), (query_second, key_second, DKB))
    for group_idx in range(2):
        query_all, key_all, key_width = groups[group_idx]
        query_heads = query_all.reshape(SEQ, HEADS, 2, key_width)
        key_heads = key_all.reshape(SEQ, HEADS, 2, key_width)
        value_heads = values[:, group_idx].reshape(SEQ, HEADS, DV)
        outputs = []
        for head in range(HEADS):
            outputs.append(one_head(query_heads[:, head], key_heads[:, head], value_heads[:, head], lambdas[group_idx, head], key_width))
        attended = jnp.concatenate(outputs, axis=1)
        mixed = mixed + jnp.dot(attended, out_weight[group_idx], preferred_element_type=jnp.float32)
    stream = residual.astype(jnp.float32) + mixed
    scale = lax.rsqrt(lax.optimization_barrier(jnp.mean(stream * stream, axis=1, keepdims=True)) + 1e-06)
    normed = (stream * scale * norm_gain.astype(jnp.float32)).astype(jnp.bfloat16)
    gate = jnp.dot(normed, gate_weight, preferred_element_type=jnp.float32)
    up_part = jnp.dot(normed, up_weight, preferred_element_type=jnp.float32)
    hidden = (jax.nn.silu(gate) * up_part).astype(jnp.bfloat16)
    ffn = jnp.dot(hidden, down_weight, preferred_element_type=jnp.float32)
    return (stream + 0.5 * ffn).astype(jnp.bfloat16)
```

```python
import functools

import jax
import jax.numpy as jnp
from jax import lax
from jax.experimental import pallas as pl
from jax.experimental.pallas import tpu as pltpu
from jax.sharding import PartitionSpec as P

D = 2048


def per_device(
    query_first,
    key_first,
    query_second,
    key_second,
    values,
    lambdas,
    residual,
    norm_gain,
    out_weight,
    gate_weight,
    up_weight,
    down_weight,
):
    tok_rows = query_first.shape[0]
    heads_here = lambdas.shape[1]
    width_first = query_first.shape[1] // (2 * heads_here)
    width_second = query_second.shape[1] // (2 * heads_here)
    value_size = values.shape[2] // heads_here
    offset = lax.axis_index("sp") * tok_rows
    query_pos = offset + lax.broadcasted_iota(jnp.int32, (tok_rows, 1), 0)
    query_groups = (
        query_first.reshape(tok_rows, heads_here, 2, width_first),
        query_second.reshape(tok_rows, heads_here, 2, width_second),
    )
    key_widths = (width_first, width_second)
    start_state = (
        jnp.full((heads_here, 2, tok_rows, 1), -1e30, jnp.float32),
        jnp.zeros((heads_here, 2, tok_rows, 1), jnp.float32),
        jnp.zeros((heads_here, 2, tok_rows, value_size), jnp.float32),
    )
    states = (start_state, start_state)
    pieces = (
        lax.all_gather(key_first, "sp", axis=0, tiled=True),
        lax.all_gather(key_second, "sp", axis=0, tiled=True),
        lax.all_gather(values, "sp", axis=0, tiled=True),
    )
    piece_rows = pieces[0].shape[0]
    key_pos = lax.broadcasted_iota(jnp.int32, (1, piece_rows), 1)
    allowed = key_pos <= query_pos
    value_rows = pieces[2].reshape(piece_rows, 2, heads_here, value_size)
    results = []
    for group_idx in range(2):
        key_width = key_widths[group_idx]
        key_part = pieces[group_idx].reshape(piece_rows, heads_here, 2, key_width)
        scores = jnp.einsum(
            "qhmd,khmd->hmqk", query_groups[group_idx], key_part, preferred_element_type=jnp.float32
        ) * key_width ** (-0.5)
        scores = jnp.where(allowed, scores, -1e30)
        running, totals, weighted = states[group_idx]
        new_peak = jnp.maximum(running, jnp.max(scores, axis=-1, keepdims=True))
        weights = jnp.where(allowed, jnp.exp(scores - new_peak), 0.0)
        totals = jnp.sum(weights, axis=-1, keepdims=True)
        weighted = jnp.einsum(
            "hmqk,khe->hmqe",
            weights.astype(jnp.bfloat16),
            value_rows[:, group_idx],
            preferred_element_type=jnp.float32,
        )
        results.append((new_peak, totals, weighted))
    states = (results[0], results[1])
    map_out = jnp.stack([states[0][2] / states[0][1], states[1][2] / states[1][1]])
    differ = map_out[:, :, 0] - lambdas[:, :, None, None] * map_out[:, :, 1]
    head_scale = lax.rsqrt(jnp.mean(differ * differ, axis=-1, keepdims=True) + 1e-06)
    attended = (0.8 * differ * head_scale).astype(jnp.bfloat16)
    projection = out_weight.reshape(2, heads_here, value_size, out_weight.shape[2])
    mixed_part = jnp.einsum(
        "ghqe,gher->qr", attended, projection, preferred_element_type=jnp.float32
    )
    mixed = lax.psum_scatter(
        mixed_part.astype(jnp.bfloat16), "tp", scatter_dimension=1, tiled=True
    ).astype(jnp.float32)
    stream = residual.astype(jnp.float32) + mixed
    squares = lax.psum(jnp.sum(stream * stream, axis=1), "tp")
    row_scale = lax.rsqrt(squares[:, None] / D + 1e-06)
    normed = (stream * row_scale * norm_gain.astype(jnp.float32)).astype(jnp.bfloat16)
    full_rows = lax.all_gather(normed, "tp", axis=1, tiled=True)
    pieces = (
        lax.all_gather(gate_weight, "sp", axis=0, tiled=True),
        lax.all_gather(up_weight, "sp", axis=0, tiled=True),
    )
    gate = jnp.dot(full_rows, pieces[0], preferred_element_type=jnp.float32)
    up_part = jnp.dot(full_rows, pieces[1], preferred_element_type=jnp.float32)
    hidden = (jax.nn.silu(gate) * up_part).astype(jnp.bfloat16)
    partial_out = jnp.dot(
        hidden,
        lax.all_gather(down_weight, "sp", axis=1, tiled=True),
        preferred_element_type=jnp.float32,
    )
    ffn = lax.psum_scatter(
        partial_out.astype(jnp.bfloat16), "tp", scatter_dimension=1, tiled=True
    ).astype(jnp.float32)
    return (stream + 0.5 * ffn).astype(jnp.bfloat16)


def flip(index, bits):
    bit = 1
    while bit <= bits:
        if (bits // bit) % 2:
            index = index + bit - 2 * bit * ((index // bit) % 2)
        bit *= 2
    return index


def nt_dot(a, b):
    return lax.dot_general(a, b, (((1,), (1,)), ((), ())), preferred_element_type=jnp.float32)


def dot(a, b):
    return jnp.dot(a, b, preferred_element_type=jnp.float32)


def layer_kernel(
    sp_count,
    widths,
    q_ref,
    kv_ref,
    lam_ref,
    residual_ref,
    gain_ref,
    proj_ref,
    gate_ref,
    up_ref,
    down_ref,
    out_ref,
    kvb,
    peak,
    total,
    acc,
    wg,
    wu,
    wd,
    mp,
    rsb,
    stream,
    act,
    gains,
    hid,
    c1,
    c1r,
    po,
    c2,
    c2r,
    c3,
    c3r,
    kv_ss,
    kv_rs,
    w_ss,
    w_rs,
    f_ss,
    f_rs,
    own_sem,
    g_ss,
    g_rs,
    rs_ss,
    rs_rs,
    az_ss,
    az_rs,
    ax_ss,
    ax_rs,
    ac_ss,
    ac_rs,
    c_ss,
    c_rs,
):
    s = lax.axis_index("sp")
    t = lax.axis_index("tp")
    y = lax.axis_index("grp")
    rows, blk = residual_ref.shape
    cols = wg.shape[2]
    hidden_all = gate_ref.shape[1]
    value_size = acc.shape[2]
    xpeer, cpeer, dpeer = flip(t, 2), flip(t, 1), flip(t, 3)
    others = range(1, sp_count)

    def remote(src, dst, ssem, rsem, **where):
        return pltpu.make_async_remote_copy(
            src_ref=src,
            dst_ref=dst,
            send_sem=ssem,
            recv_sem=rsem,
            device_id=where,
            device_id_type=pl.DeviceIdType.MESH,
        )

    barrier = pltpu.get_barrier_semaphore()
    for k in others:
        pl.semaphore_signal(barrier, inc=1, device_id={"sp": flip(s, k)}, device_id_type=pl.DeviceIdType.MESH)
        pl.semaphore_signal(barrier, inc=1, device_id={"tp": flip(t, k)}, device_id_type=pl.DeviceIdType.MESH)
    pl.semaphore_signal(barrier, inc=1, device_id={"grp": 1 - y}, device_id_type=pl.DeviceIdType.MESH)
    pl.semaphore_wait(barrier, 2 * (sp_count - 1) + 1)

    sends = []

    kv_copies = {}
    for k in others:
        copy = remote(kv_ref, kvb.at[k], kv_ss.at[k], kv_rs.at[k], sp=flip(s, k))
        kv_copies[k] = copy

        @pl.when(flip(s, k) > s)
        def _(copy=copy):
            copy.start()

    def start_of(index):
        return pl.multiple_of(jnp.minimum(index * cols, hidden_all - cols), 128)

    half_d = wg.shape[1] // 2
    half_c = cols // 2
    d_half = pl.ds(pl.multiple_of(y * half_d, half_d), half_d)
    c_half = pl.ds(pl.multiple_of(y * half_c, half_c), half_c)
    w_copies = {}
    for kind, (src, dst) in enumerate(((gate_ref, wg), (up_ref, wu), (down_ref, wd))):
        for k in others:
            begin = start_of(flip(s, k))
            if kind < 2:
                piece, place = src.at[d_half, pl.ds(begin, cols)], dst.at[s, d_half]
            else:
                piece = src.at[pl.ds(pl.multiple_of(begin + y * half_c, 64), half_c), :]
                place = dst.at[s, c_half]
            w_copies[kind, k] = remote(piece, place, w_ss.at[kind, k], w_rs.at[kind, k], sp=flip(s, k))
    for kinds in ((0, 1), (2,)):
        for k in others:
            for kind in kinds:
                w_copies[kind, k].start()
                sends.append(w_copies[kind, k])
    begin = start_of(s)
    own = [
        pltpu.make_async_copy(gate_ref.at[:, pl.ds(begin, cols)], wg.at[s], own_sem.at[0]),
        pltpu.make_async_copy(up_ref.at[:, pl.ds(begin, cols)], wu.at[s], own_sem.at[1]),
        pltpu.make_async_copy(down_ref.at[pl.ds(begin, cols), :], wd.at[s], own_sem.at[2]),
    ]
    for copy in own:
        copy.start()

    gain_copies = []
    for k in others:
        copy = remote(gain_ref, gains.at[t], g_ss.at[k], g_rs.at[k], tp=flip(t, k))
        copy.start()
        gain_copies.append(copy)
        sends.append(copy)
    gains[t] = gain_ref[...]

    q_at = (0, 2 * widths[0])
    v_at = 2 * widths[0] + 2 * widths[1]
    lane = lax.broadcasted_iota(jnp.int32, (1, 2 * widths[0]), 1)

    def block(read, diagonal):
        for group in range(2):
            width = widths[group]
            values = read(v_at + group * value_size, value_size)
            for m in range(2):
                if width % 128:
                    span = (q_at[group], 2 * width)
                    queries = q_ref[:, span[0] : span[0] + span[1]]
                    queries = jnp.where(lane // width == m, queries.astype(jnp.float32), 0.0).astype(jnp.bfloat16)
                else:
                    span = (q_at[group] + m * width, width)
                    queries = q_ref[:, span[0] : span[0] + span[1]]
                scores = nt_dot(queries, read(*span)) * width ** (-0.5)
                state = 2 * group + m
                if diagonal:
                    allowed = lax.broadcasted_iota(jnp.int32, (rows, rows), 1) <= lax.broadcasted_iota(
                        jnp.int32, (rows, rows), 0
                    )
                    scores = jnp.where(allowed, scores, -1e30)
                    top = jnp.max(scores, axis=1, keepdims=True)
                    weights = jnp.exp(scores - top)
                    peak[state] = top
                    total[state] = jnp.sum(weights, axis=1, keepdims=True)
                    acc[state] = dot(weights.astype(jnp.bfloat16), values)
                else:
                    before = peak[state]
                    top = jnp.maximum(before, jnp.max(scores, axis=1, keepdims=True))
                    fade = jnp.exp(before - top)
                    weights = jnp.exp(scores - top)
                    peak[state] = top
                    total[state] = total[state] * fade + jnp.sum(weights, axis=1, keepdims=True)
                    acc[state] = acc[state] * fade + dot(weights.astype(jnp.bfloat16), values)

    block(lambda at, size: kv_ref[:, at : at + size], True)
    for k in others:

        @pl.when(flip(s, k) < s)
        def _(k=k):
            kv_copies[k].wait_recv()
            block(lambda at, size: kvb[k, :, at : at + size], False)

    attended = []
    for group in range(2):
        first = acc[2 * group] / total[2 * group]
        second = acc[2 * group + 1] / total[2 * group + 1]
        differ = first - lam_ref[group, 0] * second
        scale = lax.rsqrt(jnp.mean(differ * differ, axis=1, keepdims=True) + 1e-06)
        attended.append((0.8 * differ * scale).astype(jnp.bfloat16))

    def project(owner):
        columns = pl.ds(pl.multiple_of(owner * blk, blk), blk)
        return dot(attended[0], proj_ref[:value_size, columns]) + dot(attended[1], proj_ref[value_size:, columns])

    rs_copies = {}
    for k in (2, 3, 1):
        mp[k] = project(flip(t, k)).astype(jnp.bfloat16)
        rs_copies[k] = remote(mp.at[k], rsb.at[k], rs_ss.at[k], rs_rs.at[k], tp=flip(t, k))
        rs_copies[k].start()
        sends.append(rs_copies[k])
    mixed = project(t)
    for k in (1, 2, 3):
        rs_copies[k].wait_recv()
        mixed = mixed + rsb[k].astype(jnp.float32)
    stream[...] = residual_ref[...].astype(jnp.float32) + mixed
    act[t, s] = stream[...].astype(jnp.bfloat16)

    az, ax, ac0, ac1 = {}, {}, {}, {}
    for k in range(sp_count):
        row = flip(s, k)
        if k:
            az[k] = remote(act.at[t, s], act.at[t, s], az_ss.at[k], az_rs.at[k], sp=row)
        ax[k] = remote(act.at[t, row], act.at[t, row], ax_ss.at[k], ax_rs.at[k], tp=xpeer)
        ac0[k] = remote(act.at[t, row], act.at[t, row], ac_ss.at[0, k], ac_rs.at[0, k], tp=cpeer)
        ac1[k] = remote(act.at[xpeer, row], act.at[xpeer, row], ac_ss.at[1, k], ac_rs.at[1, k], tp=cpeer)
    for k in others:
        az[k].start()

    def pass_on(k):
        if k:
            az[k].wait_recv()
        ax[k].start()
        ac0[k].start()

    def pass_inside(k):
        ax[k].wait_recv()
        ac1[k].start()

    fw = {}

    def hand_over(kind, k):
        w_copies[kind, k].wait_recv()
        buffer = (wg, wu, wd)[kind]
        piece = buffer.at[flip(s, k), d_half if kind < 2 else c_half]
        fw[kind, k] = remote(piece, piece, f_ss.at[kind, k], f_rs.at[kind, k], grp=1 - y)
        fw[kind, k].start()
        sends.append(fw[kind, k])

    pass_on(0)
    for k in others:
        for kind in (0, 1):
            hand_over(kind, k)
        pass_on(k)
        pass_inside(k - 1)
    for k in others:
        hand_over(2, k)
    pass_inside(sp_count - 1)

    for copy in gain_copies:
        copy.wait_recv()
    for kind in (0, 1):
        own[kind].wait()
        for k in others:
            fw[kind, k].wait_recv()
    column = start_of(s) + lax.broadcasted_iota(jnp.int32, (1, cols), 1)
    mine = column >= s * cols

    def hidden_of(k):
        row = flip(s, k)
        ac0[k].wait_recv()
        ac1[k].wait_recv()
        squares = jnp.zeros((rows, 1), jnp.float32)
        for part in range(sp_count):
            piece = act[part, row].astype(jnp.float32)
            squares = squares + jnp.sum(piece * piece, axis=1, keepdims=True)
        scale = lax.rsqrt(squares / (sp_count * blk) + 1e-06)
        gate = jnp.zeros((rows, cols), jnp.float32)
        up = jnp.zeros((rows, cols), jnp.float32)
        for part in range(sp_count):
            gain = gains[part, 0:1, :].astype(jnp.float32)
            normed = (act[part, row].astype(jnp.float32) * scale * gain).astype(jnp.bfloat16)
            gate = gate + dot(normed, wg[part])
            up = up + dot(normed, wu[part])
        hidden = gate / (1.0 + jnp.exp(-gate)) * up
        hid[k] = jnp.where(mine, hidden, 0.0).astype(jnp.bfloat16)

    r1, r2, r3 = {}, {}, {}
    for k in range(sp_count):
        r1[k] = remote(c1.at[k], c1r.at[k], c_ss.at[0, k], c_rs.at[0, k], tp=cpeer)
        r2[k] = remote(c2.at[k], c2r.at[k], c_ss.at[1, k], c_rs.at[1, k], tp=xpeer)
        if k:
            r3[k] = remote(c3.at[k], c3r.at[k], c_ss.at[2, k], c_rs.at[2, k], sp=flip(s, k))

    def down_of(k):
        hidden = hid[k]
        c1[k, 0] = dot(hidden, wd[cpeer]).astype(jnp.bfloat16)
        c1[k, 1] = dot(hidden, wd[dpeer]).astype(jnp.bfloat16)
        r1[k].start()
        po[k, 1] = dot(hidden, wd[xpeer])
        po[k, 0] = dot(hidden, wd[t])

    def across(k):
        r1[k].wait_recv()
        c2[k] = (po[k, 1] + c1r[k, 1].astype(jnp.float32)).astype(jnp.bfloat16)
        r2[k].start()

    def along(k):
        r2[k].wait_recv()
        result = po[k, 0] + c1r[k, 0].astype(jnp.float32) + c2r[k].astype(jnp.float32)
        if k:
            c3[k] = result.astype(jnp.bfloat16)
            r3[k].start()
        else:
            po[0, 0] = result

    order = (3, 2, 1, 0)
    first = True
    for at, k in enumerate(order):
        hidden_of(k)
        if first:
            own[2].wait()
            for j in others:
                fw[2, j].wait_recv()
            first = False
        down_of(k)
        if at >= 1:
            across(order[at - 1])
        if at >= 2:
            along(order[at - 2])
    across(order[-1])
    along(order[-2])
    along(order[-1])

    ffn = po[0, 0]
    for k in order[:-1]:
        r3[k].wait_recv()
        ffn = ffn + c3r[k].astype(jnp.float32)
    out_ref[...] = (stream[...] + 0.5 * ffn).astype(jnp.bfloat16)

    for k in others:

        @pl.when(flip(s, k) > s)
        def _(k=k):
            kv_copies[k].wait_send()

    for copies in (az, ax, ac0, ac1, r1, r2, r3):
        sends.extend(copies.values())
    for copy in sends:
        copy.wait_send()


def fits(axes, query_first, values, lambdas, residual, gate_weight):
    sp, tp = axes["sp"], axes["tp"]
    rows, blk = residual.shape
    depth, hidden_all = gate_weight.shape
    if axes["grp"] != 2 or sp != tp or tp != 4 or lambdas.shape[1] != 1:
        return False
    if depth != blk or blk % 128 or hidden_all % 128 or rows % 16:
        return False
    if (2 * query_first.shape[1]) % 256 or values.shape[2] % 128:
        return False
    cols = -(-hidden_all // (128 * sp)) * 128
    if cols * sp - hidden_all >= cols or cols > hidden_all:
        return False
    need = 6 * sp * blk * cols + rows * blk * 2 * 20 * sp
    return need < 40 * 1024 * 1024


def one_device(
    axes,
    query_first,
    key_first,
    query_second,
    key_second,
    values,
    lambdas,
    residual,
    norm_gain,
    out_weight,
    gate_weight,
    up_weight,
    down_weight,
):
    if not fits(axes, query_first, values, lambdas, residual, gate_weight):
        return per_device(
            query_first,
            key_first,
            query_second,
            key_second,
            values,
            lambdas,
            residual,
            norm_gain,
            out_weight,
            gate_weight,
            up_weight,
            down_weight,
        )
    n = axes["sp"]
    rows, blk = residual.shape
    hidden_all = gate_weight.shape[1]
    cols = -(-hidden_all // (128 * n)) * 128
    value_size = values.shape[2]
    widths = (query_first.shape[1] // 2, query_second.shape[1] // 2)
    queries = jnp.concatenate([query_first, query_second], axis=1)
    kv = jnp.concatenate([key_first, key_second, values[:, 0], values[:, 1]], axis=1)
    gain = jnp.broadcast_to(norm_gain[None, :], (16, blk))
    projection = out_weight.reshape(2 * value_size, out_weight.shape[2])
    bf16, f32 = jnp.bfloat16, jnp.float32
    vmem = pl.BlockSpec(memory_space=pltpu.VMEM)
    smem = pl.BlockSpec(memory_space=pltpu.SMEM)
    hbm = pl.BlockSpec(memory_space=pl.ANY)
    dma = pltpu.SemaphoreType.DMA
    return pl.pallas_call(
        functools.partial(layer_kernel, n, widths),
        out_shape=jax.ShapeDtypeStruct((rows, blk), bf16),
        in_specs=[vmem, vmem, smem, vmem, vmem, vmem, hbm, hbm, hbm],
        out_specs=vmem,
        scratch_shapes=[
            pltpu.VMEM((n,) + kv.shape, bf16),
            pltpu.VMEM((4, rows, 1), f32),
            pltpu.VMEM((4, rows, 1), f32),
            pltpu.VMEM((4, rows, value_size), f32),
            pltpu.VMEM((n, blk, cols), bf16),
            pltpu.VMEM((n, blk, cols), bf16),
            pltpu.VMEM((n, cols, blk), bf16),
            pltpu.VMEM((n, rows, blk), bf16),
            pltpu.VMEM((n, rows, blk), bf16),
            pltpu.VMEM((rows, blk), f32),
            pltpu.VMEM((n, n, rows, blk), bf16),
            pltpu.VMEM((n, 16, blk), bf16),
            pltpu.VMEM((n, rows, cols), bf16),
            pltpu.VMEM((n, 2, rows, blk), bf16),
            pltpu.VMEM((n, 2, rows, blk), bf16),
            pltpu.VMEM((n, 2, rows, blk), f32),
            pltpu.VMEM((n, rows, blk), bf16),
            pltpu.VMEM((n, rows, blk), bf16),
            pltpu.VMEM((n, rows, blk), bf16),
            pltpu.VMEM((n, rows, blk), bf16),
            dma((n,)),
            dma((n,)),
            dma((3, n)),
            dma((3, n)),
            dma((3, n)),
            dma((3, n)),
            dma((3,)),
            dma((n,)),
            dma((n,)),
            dma((n,)),
            dma((n,)),
            dma((n,)),
            dma((n,)),
            dma((n,)),
            dma((n,)),
            dma((2, n)),
            dma((2, n)),
            dma((3, n)),
            dma((3, n)),
        ],
        compiler_params=pltpu.CompilerParams(
            collective_id=0, has_side_effects=True, vmem_limit_bytes=60 * 1024 * 1024
        ),
    )(queries, kv, lambdas, residual, gain, projection, gate_weight, up_weight, down_weight)

def solution(mesh):
    return jax.shard_map(
        functools.partial(one_device, dict(mesh.shape)),
        mesh=mesh,
        in_specs=(
            P(("grp", "sp"), "tp"),
            P(("grp", "sp"), "tp"),
            P(("grp", "sp"), "tp"),
            P(("grp", "sp"), "tp"),
            P(("grp", "sp"), None, "tp"),
            P(None, "tp"),
            P(("grp", "sp"), "tp"),
            P("tp"),
            P(None, "tp", None),
            P("sp", "tp"),
            P("sp", "tp"),
            P("tp", "sp"),
        ),
        out_specs=P(("grp", "sp"), "tp"),
        check_vma=False,
    )
```

```python
import functools

import jax
import jax.numpy as jnp
from jax import lax
from jax.experimental import pallas as pl
from jax.experimental.pallas import tpu as pltpu
from jax.sharding import PartitionSpec as P

D = 2048


def per_device(
    query_first,
    key_first,
    query_second,
    key_second,
    values,
    lambdas,
    residual,
    norm_gain,
    out_weight,
    gate_weight,
    up_weight,
    down_weight,
):
    tok_rows = query_first.shape[0]
    heads_here = lambdas.shape[1]
    width_first = query_first.shape[1] // (2 * heads_here)
    width_second = query_second.shape[1] // (2 * heads_here)
    value_size = values.shape[2] // heads_here
    offset = lax.axis_index("sp") * tok_rows
    query_pos = offset + lax.broadcasted_iota(jnp.int32, (tok_rows, 1), 0)
    query_groups = (
        query_first.reshape(tok_rows, heads_here, 2, width_first),
        query_second.reshape(tok_rows, heads_here, 2, width_second),
    )
    key_widths = (width_first, width_second)
    start_state = (
        jnp.full((heads_here, 2, tok_rows, 1), -1e30, jnp.float32),
        jnp.zeros((heads_here, 2, tok_rows, 1), jnp.float32),
        jnp.zeros((heads_here, 2, tok_rows, value_size), jnp.float32),
    )
    states = (start_state, start_state)
    pieces = (
        lax.all_gather(key_first, "sp", axis=0, tiled=True),
        lax.all_gather(key_second, "sp", axis=0, tiled=True),
        lax.all_gather(values, "sp", axis=0, tiled=True),
    )
    piece_rows = pieces[0].shape[0]
    key_pos = lax.broadcasted_iota(jnp.int32, (1, piece_rows), 1)
    allowed = key_pos <= query_pos
    value_rows = pieces[2].reshape(piece_rows, 2, heads_here, value_size)
    results = []
    for group_idx in range(2):
        key_width = key_widths[group_idx]
        key_part = pieces[group_idx].reshape(piece_rows, heads_here, 2, key_width)
        scores = jnp.einsum(
            "qhmd,khmd->hmqk", query_groups[group_idx], key_part, preferred_element_type=jnp.float32
        ) * key_width ** (-0.5)
        scores = jnp.where(allowed, scores, -1e30)
        running, totals, weighted = states[group_idx]
        new_peak = jnp.maximum(running, jnp.max(scores, axis=-1, keepdims=True))
        weights = jnp.where(allowed, jnp.exp(scores - new_peak), 0.0)
        totals = jnp.sum(weights, axis=-1, keepdims=True)
        weighted = jnp.einsum(
            "hmqk,khe->hmqe",
            weights.astype(jnp.bfloat16),
            value_rows[:, group_idx],
            preferred_element_type=jnp.float32,
        )
        results.append((new_peak, totals, weighted))
    states = (results[0], results[1])
    map_out = jnp.stack([states[0][2] / states[0][1], states[1][2] / states[1][1]])
    differ = map_out[:, :, 0] - lambdas[:, :, None, None] * map_out[:, :, 1]
    head_scale = lax.rsqrt(jnp.mean(differ * differ, axis=-1, keepdims=True) + 1e-06)
    attended = (0.8 * differ * head_scale).astype(jnp.bfloat16)
    projection = out_weight.reshape(2, heads_here, value_size, out_weight.shape[2])
    mixed_part = jnp.einsum(
        "ghqe,gher->qr", attended, projection, preferred_element_type=jnp.float32
    )
    mixed = lax.psum_scatter(
        mixed_part.astype(jnp.bfloat16), "tp", scatter_dimension=1, tiled=True
    ).astype(jnp.float32)
    stream = residual.astype(jnp.float32) + mixed
    squares = lax.psum(jnp.sum(stream * stream, axis=1), "tp")
    row_scale = lax.rsqrt(squares[:, None] / D + 1e-06)
    normed = (stream * row_scale * norm_gain.astype(jnp.float32)).astype(jnp.bfloat16)
    full_rows = lax.all_gather(normed, "tp", axis=1, tiled=True)
    pieces = (
        lax.all_gather(gate_weight, "sp", axis=0, tiled=True),
        lax.all_gather(up_weight, "sp", axis=0, tiled=True),
    )
    gate = jnp.dot(full_rows, pieces[0], preferred_element_type=jnp.float32)
    up_part = jnp.dot(full_rows, pieces[1], preferred_element_type=jnp.float32)
    hidden = (jax.nn.silu(gate) * up_part).astype(jnp.bfloat16)
    partial_out = jnp.dot(
        hidden,
        lax.all_gather(down_weight, "sp", axis=1, tiled=True),
        preferred_element_type=jnp.float32,
    )
    ffn = lax.psum_scatter(
        partial_out.astype(jnp.bfloat16), "tp", scatter_dimension=1, tiled=True
    ).astype(jnp.float32)
    return (stream + 0.5 * ffn).astype(jnp.bfloat16)


def flip(index, bits):
    bit = 1
    while bit <= bits:
        if (bits // bit) % 2:
            index = index + bit - 2 * bit * ((index // bit) % 2)
        bit *= 2
    return index


def nt_dot(a, b):
    return lax.dot_general(a, b, (((1,), (1,)), ((), ())), preferred_element_type=jnp.float32)


def dot(a, b):
    return jnp.dot(a, b, preferred_element_type=jnp.float32)


def layer_kernel(
    sp_count,
    widths,
    q1_ref,
    q2_ref,
    k1_ref,
    k2_ref,
    v_ref,
    lam_ref,
    residual_ref,
    gain_ref,
    proj_hbm,
    gate_ref,
    up_ref,
    down_ref,
    out_ref,
    k1b,
    k2b,
    vb,
    proj_ref,
    peak,
    total,
    acc,
    wg,
    wu,
    wd,
    mp,
    rsb,
    stream,
    act,
    gains,
    hid,
    c1,
    c1r,
    po,
    c2,
    c2r,
    c3,
    c3r,
    kv_ss,
    kv_rs,
    w_ss,
    w_rs,
    f_ss,
    f_rs,
    own_sem,
    g_ss,
    g_rs,
    rs_ss,
    rs_rs,
    az_ss,
    az_rs,
    ax_ss,
    ax_rs,
    ac_ss,
    ac_rs,
    c_ss,
    c_rs,
):
    s = lax.axis_index("sp")
    t = lax.axis_index("tp")
    y = lax.axis_index("grp")
    rows, blk = residual_ref.shape
    cols = wg.shape[2]
    hidden_all = gate_ref.shape[1]
    value_size = acc.shape[2]
    xpeer, cpeer, dpeer = flip(t, 2), flip(t, 1), flip(t, 3)
    others = range(1, sp_count)

    def remote(src, dst, ssem, rsem, **where):
        return pltpu.make_async_remote_copy(
            src_ref=src,
            dst_ref=dst,
            send_sem=ssem,
            recv_sem=rsem,
            device_id=where,
            device_id_type=pl.DeviceIdType.MESH,
        )

    barrier = pltpu.get_barrier_semaphore()
    for k in others:
        pl.semaphore_signal(barrier, inc=1, device_id={"sp": flip(s, k)}, device_id_type=pl.DeviceIdType.MESH)
        pl.semaphore_signal(barrier, inc=1, device_id={"tp": flip(t, k)}, device_id_type=pl.DeviceIdType.MESH)
    pl.semaphore_signal(barrier, inc=1, device_id={"grp": 1 - y}, device_id_type=pl.DeviceIdType.MESH)
    pl.semaphore_wait(barrier, 2 * (sp_count - 1) + 1)

    sends = []

    kv_copies = {}
    for k in others:
        kv_copies[k] = [
            remote(src, dst.at[k], kv_ss.at[i, k], kv_rs.at[i, k], sp=flip(s, k))
            for i, (src, dst) in enumerate(((k1_ref, k1b), (k2_ref, k2b), (v_ref, vb)))
        ]

        @pl.when(flip(s, k) > s)
        def _(k=k):
            for copy in kv_copies[k]:
                copy.start()

    half_d = wg.shape[1] // 2
    half_c = cols // 2
    extra = sp_count * cols - hidden_all
    half_last = (cols - extra) // 2
    d_half = pl.ds(pl.multiple_of(y * half_d, half_d), half_d)
    last = sp_count - 1

    def w_copy(kind, k, source, target, short):
        src, dst = ((gate_ref, wg), (up_ref, wu), (down_ref, wd))[kind]
        begin = hidden_all - cols + extra if short else pl.multiple_of(target * cols, 128)
        skip, size = (extra, cols - extra) if short else (0, cols)
        if kind < 2:
            piece = src.at[d_half, pl.ds(begin, size)]
            place = dst.at[source, d_half, pl.ds(skip, size)]
        else:
            part = y * (size // 2)
            piece = src.at[pl.ds(pl.multiple_of(begin + part, 64), size // 2), :]
            place = dst.at[source, pl.ds(pl.multiple_of(skip + part, 64), size // 2)]
        return remote(piece, place, w_ss.at[kind, k], w_rs.at[kind, k], sp=flip(s, k)), place

    def f_copy(kind, k, short):
        _, place = w_copy(kind, k, flip(s, k), s, short)
        return remote(place, place, f_ss.at[kind, k], f_rs.at[kind, k], grp=1 - y)

    def either(test, action):
        pl.when(test)(lambda: action(True))
        pl.when(jnp.logical_not(test))(lambda: action(False))

    def send_weights(kinds):
        for k in others:

            def go(short, k=k):
                for kind in kinds:
                    w_copy(kind, k, s, flip(s, k), short)[0].start()

            either(flip(s, k) == last, go)

    @pl.when(s == last)
    def _():
        wg[:, :, :extra] = jnp.zeros((sp_count, wg.shape[1], extra), jnp.bfloat16)
        wu[:, :, :extra] = jnp.zeros((sp_count, wg.shape[1], extra), jnp.bfloat16)
        wd[:, :extra, :] = jnp.zeros((sp_count, extra, blk), jnp.bfloat16)

    send_weights((0, 1))
    proj_copy = pltpu.make_async_copy(proj_hbm, proj_ref, own_sem.at[3])
    proj_copy.start()
    def own_copy(kind, short):
        src, dst = ((gate_ref, wg), (up_ref, wu), (down_ref, wd))[kind]
        begin = hidden_all - cols + extra if short else pl.multiple_of(s * cols, 128)
        skip, size = (extra, cols - extra) if short else (0, cols)
        if kind < 2:
            return pltpu.make_async_copy(src.at[:, pl.ds(begin, size)], dst.at[s, :, pl.ds(skip, size)], own_sem.at[kind])
        return pltpu.make_async_copy(src.at[pl.ds(begin, size), :], dst.at[s, pl.ds(skip, size)], own_sem.at[kind])

    def start_own(short):
        for kind in range(3):
            own_copy(kind, short).start()

    either(s == last, start_own)

    gains[t] = jnp.broadcast_to(gain_ref[...].reshape(1, blk), gains.shape[1:])
    gain_copies = []
    for k in others:
        copy = remote(gains.at[t], gains.at[t], g_ss.at[k], g_rs.at[k], tp=flip(t, k))
        copy.start()
        gain_copies.append(copy)
        sends.append(copy)

    q_refs = (q1_ref, q2_ref)
    lane = lax.broadcasted_iota(jnp.int32, (1, 2 * widths[0]), 1)

    def block(keys, v, diagonal):
        for group in range(2):
            width = widths[group]
            values = v[:, group, :]
            for m in range(2):
                if width % 128:
                    span = slice(0, 2 * width)
                    queries = q_refs[group][:, span]
                    queries = jnp.where(lane // width == m, queries.astype(jnp.float32), 0.0).astype(jnp.bfloat16)
                else:
                    span = slice(m * width, (m + 1) * width)
                    queries = q_refs[group][:, span]
                scores = nt_dot(queries, keys[group][:, span]) * width ** (-0.5)
                state = 2 * group + m
                if diagonal:
                    allowed = lax.broadcasted_iota(jnp.int32, (rows, rows), 1) <= lax.broadcasted_iota(
                        jnp.int32, (rows, rows), 0
                    )
                    scores = jnp.where(allowed, scores, -1e30)
                    top = jnp.max(scores, axis=1, keepdims=True)
                    weights = jnp.exp(scores - top)
                    peak[state] = top
                    total[state] = jnp.sum(weights, axis=1, keepdims=True)
                    acc[state] = dot(weights.astype(jnp.bfloat16), values)
                else:
                    before = peak[state]
                    top = jnp.maximum(before, jnp.max(scores, axis=1, keepdims=True))
                    fade = jnp.exp(before - top)
                    weights = jnp.exp(scores - top)
                    peak[state] = top
                    total[state] = total[state] * fade + jnp.sum(weights, axis=1, keepdims=True)
                    acc[state] = acc[state] * fade + dot(weights.astype(jnp.bfloat16), values)

    block((k1_ref, k2_ref), v_ref, True)
    for k in others:

        @pl.when(flip(s, k) < s)
        def _(k=k):
            for copy in kv_copies[k]:
                copy.wait_recv()
            block((k1b.at[k], k2b.at[k]), vb.at[k], False)

    proj_copy.wait()
    attended = []
    for group in range(2):
        first = acc[2 * group] / total[2 * group]
        second = acc[2 * group + 1] / total[2 * group + 1]
        differ = first - lam_ref[0, group] * second
        scale = lax.rsqrt(jnp.mean(differ * differ, axis=1, keepdims=True) + 1e-06)
        attended.append((0.8 * differ * scale).astype(jnp.bfloat16))

    def project(owner):
        columns = pl.ds(pl.multiple_of(owner * blk, blk), blk)
        return dot(attended[0], proj_ref[0, :, columns]) + dot(attended[1], proj_ref[1, :, columns])

    rs_copies = {}
    for k in (2, 3, 1):
        mp[k] = project(flip(t, k)).astype(jnp.bfloat16)
        rs_copies[k] = remote(mp.at[k], rsb.at[k], rs_ss.at[k], rs_rs.at[k], tp=flip(t, k))
        rs_copies[k].start()
        sends.append(rs_copies[k])
    mixed = project(t)
    for k in (1, 2, 3):
        rs_copies[k].wait_recv()
        mixed = mixed + rsb[k].astype(jnp.float32)
    stream[...] = residual_ref[...].astype(jnp.float32) + mixed
    act[t, s] = stream[...].astype(jnp.bfloat16)

    az, ax, ac0, ac1 = {}, {}, {}, {}
    for k in range(sp_count):
        row = flip(s, k)
        if k:
            az[k] = remote(act.at[t, s], act.at[t, s], az_ss.at[k], az_rs.at[k], sp=row)
        ax[k] = remote(act.at[t, row], act.at[t, row], ax_ss.at[k], ax_rs.at[k], tp=xpeer)
        ac0[k] = remote(act.at[t, row], act.at[t, row], ac_ss.at[0, k], ac_rs.at[0, k], tp=cpeer)
        ac1[k] = remote(act.at[xpeer, row], act.at[xpeer, row], ac_ss.at[1, k], ac_rs.at[1, k], tp=cpeer)
    for k in others:
        az[k].start()
    send_weights((2,))

    def pass_on(k):
        if k:
            az[k].wait_recv()
        ax[k].start()
        ac0[k].start()

    def pass_inside(k):
        ax[k].wait_recv()
        ac1[k].start()

    def hand_over(kinds, k):
        def go(short):
            for kind in kinds:
                w_copy(kind, k, flip(s, k), s, short)[0].wait_recv()
                f_copy(kind, k, short).start()

        either(s == last, go)

    def await_weights(kinds):
        def go(short):
            for kind in kinds:
                own_copy(kind, short).wait()
                for k in others:
                    f_copy(kind, k, short).wait_recv()

        either(s == last, go)

    pass_on(0)
    for k in others:
        hand_over((0, 1), k)
        pass_on(k)
        pass_inside(k - 1)
    pass_inside(sp_count - 1)

    for copy in gain_copies:
        copy.wait_recv()
    await_weights((0, 1))
    column = jnp.minimum(s * cols, hidden_all - cols) + lax.broadcasted_iota(jnp.int32, (1, cols), 1)
    mine = column >= s * cols

    def hidden_of(k):
        row = flip(s, k)
        ac0[k].wait_recv()
        ac1[k].wait_recv()
        squares = jnp.zeros((rows, 1), jnp.float32)
        for part in range(sp_count):
            piece = act[part, row].astype(jnp.float32)
            squares = squares + jnp.sum(piece * piece, axis=1, keepdims=True)
        scale = lax.rsqrt(squares / (sp_count * blk) + 1e-06)
        gate = jnp.zeros((rows, cols), jnp.float32)
        up = jnp.zeros((rows, cols), jnp.float32)
        for part in range(sp_count):
            gain = gains[part, 0:1, :].astype(jnp.float32)
            normed = (act[part, row].astype(jnp.float32) * scale * gain).astype(jnp.bfloat16)
            gate = gate + dot(normed, wg[part])
            up = up + dot(normed, wu[part])
        hidden = gate / (1.0 + jnp.exp(-gate)) * up
        hid[k] = jnp.where(mine, hidden, 0.0).astype(jnp.bfloat16)

    r1, r2, r3 = {}, {}, {}
    for k in range(sp_count):
        r1[k] = remote(c1.at[k], c1r.at[k], c_ss.at[0, k], c_rs.at[0, k], tp=cpeer)
        r2[k] = remote(c2.at[k], c2r.at[k], c_ss.at[1, k], c_rs.at[1, k], tp=xpeer)
        if k:
            r3[k] = remote(c3.at[k], c3r.at[k], c_ss.at[2, k], c_rs.at[2, k], sp=flip(s, k))

    def down_of(k):
        hidden = hid[k]
        c1[k, 0] = dot(hidden, wd[cpeer]).astype(jnp.bfloat16)
        c1[k, 1] = dot(hidden, wd[dpeer]).astype(jnp.bfloat16)
        r1[k].start()
        po[k, 1] = dot(hidden, wd[xpeer])
        po[k, 0] = dot(hidden, wd[t])

    def across(k):
        r1[k].wait_recv()
        c2[k] = (po[k, 1] + c1r[k, 1].astype(jnp.float32)).astype(jnp.bfloat16)
        r2[k].start()

    def along(k):
        r2[k].wait_recv()
        result = po[k, 0] + c1r[k, 0].astype(jnp.float32) + c2r[k].astype(jnp.float32)
        if k:
            c3[k] = result.astype(jnp.bfloat16)
            r3[k].start()
        else:
            po[0, 0] = result

    order = (3, 2, 1, 0)
    first = True
    for at, k in enumerate(order):
        hidden_of(k)
        if first:
            for j in others:
                hand_over((2,), j)
            await_weights((2,))
            first = False
        down_of(k)
        if at >= 1:
            across(order[at - 1])
        if at >= 2:
            along(order[at - 2])
    across(order[-1])
    along(order[-2])
    along(order[-1])

    ffn = po[0, 0]
    for k in order[:-1]:
        r3[k].wait_recv()
        ffn = ffn + c3r[k].astype(jnp.float32)
    out_ref[...] = (stream[...] + 0.5 * ffn).astype(jnp.bfloat16)

    for k in others:

        @pl.when(flip(s, k) > s)
        def _(k=k):
            for copy in kv_copies[k]:
                copy.wait_send()

    def finish():
        for k in others:

            def go(short, k=k):
                for kind in range(3):
                    w_copy(kind, k, s, flip(s, k), short)[0].wait_send()

            either(flip(s, k) == last, go)

        def gone(short):
            for k in others:
                for kind in range(3):
                    f_copy(kind, k, short).wait_send()

        either(s == last, gone)

    finish()
    for copies in (az, ax, ac0, ac1, r1, r2, r3):
        sends.extend(copies.values())
    for copy in sends:
        copy.wait_send()


def fits(axes, query_first, values, lambdas, residual, gate_weight):
    sp, tp = axes["sp"], axes["tp"]
    rows, blk = residual.shape
    depth, hidden_all = gate_weight.shape
    if axes["grp"] != 2 or sp != tp or tp != 4 or lambdas.shape[1] != 1:
        return False
    if depth != blk or blk % 128 or hidden_all % 128 or rows % 16:
        return False
    if (2 * query_first.shape[1]) % 256 or values.shape[2] % 128:
        return False
    cols = -(-hidden_all // (128 * sp)) * 128
    if cols * sp - hidden_all >= cols or cols > hidden_all:
        return False
    if (cols * sp - hidden_all) % 128 or blk % 32:
        return False
    need = 6 * sp * blk * cols + rows * blk * 2 * 20 * sp
    return need < 40 * 1024 * 1024


def one_device(
    axes,
    query_first,
    key_first,
    query_second,
    key_second,
    values,
    lambdas,
    residual,
    norm_gain,
    out_weight,
    gate_weight,
    up_weight,
    down_weight,
):
    if not fits(axes, query_first, values, lambdas, residual, gate_weight):
        return per_device(
            query_first,
            key_first,
            query_second,
            key_second,
            values,
            lambdas,
            residual,
            norm_gain,
            out_weight,
            gate_weight,
            up_weight,
            down_weight,
        )
    n = axes["sp"]
    rows, blk = residual.shape
    hidden_all = gate_weight.shape[1]
    cols = -(-hidden_all // (128 * n)) * 128
    value_size = values.shape[2]
    widths = (query_first.shape[1] // 2, query_second.shape[1] // 2)
    bf16, f32 = jnp.bfloat16, jnp.float32
    vmem = pl.BlockSpec(memory_space=pltpu.VMEM)
    smem = pl.BlockSpec(memory_space=pltpu.SMEM)
    hbm = pl.BlockSpec(memory_space=pl.ANY)
    dma = pltpu.SemaphoreType.DMA
    return pl.pallas_call(
        functools.partial(layer_kernel, n, widths),
        out_shape=jax.ShapeDtypeStruct((rows, blk), bf16),
        in_specs=[vmem] * 5 + [smem, vmem, vmem] + [hbm] * 4,
        out_specs=vmem,
        scratch_shapes=[
            pltpu.VMEM((n,) + key_first.shape, bf16),
            pltpu.VMEM((n,) + key_second.shape, bf16),
            pltpu.VMEM((n,) + values.shape, bf16),
            pltpu.VMEM(out_weight.shape, bf16),
            pltpu.VMEM((4, rows, 1), f32),
            pltpu.VMEM((4, rows, 1), f32),
            pltpu.VMEM((4, rows, value_size), f32),
            pltpu.VMEM((n, blk, cols), bf16),
            pltpu.VMEM((n, blk, cols), bf16),
            pltpu.VMEM((n, cols, blk), bf16),
            pltpu.VMEM((n, rows, blk), bf16),
            pltpu.VMEM((n, rows, blk), bf16),
            pltpu.VMEM((rows, blk), f32),
            pltpu.VMEM((n, n, rows, blk), bf16),
            pltpu.VMEM((n, 16, blk), bf16),
            pltpu.VMEM((n, rows, cols), bf16),
            pltpu.VMEM((n, 2, rows, blk), bf16),
            pltpu.VMEM((n, 2, rows, blk), bf16),
            pltpu.VMEM((n, 2, rows, blk), f32),
            pltpu.VMEM((n, rows, blk), bf16),
            pltpu.VMEM((n, rows, blk), bf16),
            pltpu.VMEM((n, rows, blk), bf16),
            pltpu.VMEM((n, rows, blk), bf16),
            dma((3, n)),
            dma((3, n)),
            dma((3, n)),
            dma((3, n)),
            dma((3, n)),
            dma((3, n)),
            dma((4,)),
            dma((n,)),
            dma((n,)),
            dma((n,)),
            dma((n,)),
            dma((n,)),
            dma((n,)),
            dma((n,)),
            dma((n,)),
            dma((2, n)),
            dma((2, n)),
            dma((3, n)),
            dma((3, n)),
        ],
        compiler_params=pltpu.CompilerParams(
            collective_id=0, has_side_effects=True, vmem_limit_bytes=60 * 1024 * 1024
        ),
    )(
        query_first,
        query_second,
        key_first,
        key_second,
        values,
        lambdas.T,
        residual,
        norm_gain,
        out_weight,
        gate_weight,
        up_weight,
        down_weight,
    )

def solution(mesh):
    return jax.shard_map(
        functools.partial(one_device, dict(mesh.shape)),
        mesh=mesh,
        in_specs=(
            P(("grp", "sp"), "tp"),
            P(("grp", "sp"), "tp"),
            P(("grp", "sp"), "tp"),
            P(("grp", "sp"), "tp"),
            P(("grp", "sp"), None, "tp"),
            P(None, "tp"),
            P(("grp", "sp"), "tp"),
            P("tp"),
            P(None, "tp", None),
            P("sp", "tp"),
            P("sp", "tp"),
            P("tp", "sp"),
        ),
        out_specs=P(("grp", "sp"), "tp"),
        check_vma=False,
    )
```

```python
import functools

import jax
import jax.numpy as jnp
from jax import lax
from jax.experimental import pallas as pl
from jax.experimental.pallas import tpu as pltpu
from jax.sharding import PartitionSpec as P

D = 2048


def per_device(
    query_first,
    key_first,
    query_second,
    key_second,
    values,
    lambdas,
    residual,
    norm_gain,
    out_weight,
    gate_weight,
    up_weight,
    down_weight,
):
    tok_rows = query_first.shape[0]
    heads_here = lambdas.shape[1]
    width_first = query_first.shape[1] // (2 * heads_here)
    width_second = query_second.shape[1] // (2 * heads_here)
    value_size = values.shape[2] // heads_here
    offset = lax.axis_index("sp") * tok_rows
    query_pos = offset + lax.broadcasted_iota(jnp.int32, (tok_rows, 1), 0)
    query_groups = (
        query_first.reshape(tok_rows, heads_here, 2, width_first),
        query_second.reshape(tok_rows, heads_here, 2, width_second),
    )
    key_widths = (width_first, width_second)
    start_state = (
        jnp.full((heads_here, 2, tok_rows, 1), -1e30, jnp.float32),
        jnp.zeros((heads_here, 2, tok_rows, 1), jnp.float32),
        jnp.zeros((heads_here, 2, tok_rows, value_size), jnp.float32),
    )
    states = (start_state, start_state)
    pieces = (
        lax.all_gather(key_first, "sp", axis=0, tiled=True),
        lax.all_gather(key_second, "sp", axis=0, tiled=True),
        lax.all_gather(values, "sp", axis=0, tiled=True),
    )
    piece_rows = pieces[0].shape[0]
    key_pos = lax.broadcasted_iota(jnp.int32, (1, piece_rows), 1)
    allowed = key_pos <= query_pos
    value_rows = pieces[2].reshape(piece_rows, 2, heads_here, value_size)
    results = []
    for group_idx in range(2):
        key_width = key_widths[group_idx]
        key_part = pieces[group_idx].reshape(piece_rows, heads_here, 2, key_width)
        scores = jnp.einsum(
            "qhmd,khmd->hmqk", query_groups[group_idx], key_part, preferred_element_type=jnp.float32
        ) * key_width ** (-0.5)
        scores = jnp.where(allowed, scores, -1e30)
        running, totals, weighted = states[group_idx]
        new_peak = jnp.maximum(running, jnp.max(scores, axis=-1, keepdims=True))
        weights = jnp.where(allowed, jnp.exp(scores - new_peak), 0.0)
        totals = jnp.sum(weights, axis=-1, keepdims=True)
        weighted = jnp.einsum(
            "hmqk,khe->hmqe",
            weights.astype(jnp.bfloat16),
            value_rows[:, group_idx],
            preferred_element_type=jnp.float32,
        )
        results.append((new_peak, totals, weighted))
    states = (results[0], results[1])
    map_out = jnp.stack([states[0][2] / states[0][1], states[1][2] / states[1][1]])
    differ = map_out[:, :, 0] - lambdas[:, :, None, None] * map_out[:, :, 1]
    head_scale = lax.rsqrt(jnp.mean(differ * differ, axis=-1, keepdims=True) + 1e-06)
    attended = (0.8 * differ * head_scale).astype(jnp.bfloat16)
    projection = out_weight.reshape(2, heads_here, value_size, out_weight.shape[2])
    mixed_part = jnp.einsum(
        "ghqe,gher->qr", attended, projection, preferred_element_type=jnp.float32
    )
    mixed = lax.psum_scatter(
        mixed_part.astype(jnp.bfloat16), "tp", scatter_dimension=1, tiled=True
    ).astype(jnp.float32)
    stream = residual.astype(jnp.float32) + mixed
    squares = lax.psum(jnp.sum(stream * stream, axis=1), "tp")
    row_scale = lax.rsqrt(squares[:, None] / D + 1e-06)
    normed = (stream * row_scale * norm_gain.astype(jnp.float32)).astype(jnp.bfloat16)
    full_rows = lax.all_gather(normed, "tp", axis=1, tiled=True)
    pieces = (
        lax.all_gather(gate_weight, "sp", axis=0, tiled=True),
        lax.all_gather(up_weight, "sp", axis=0, tiled=True),
    )
    gate = jnp.dot(full_rows, pieces[0], preferred_element_type=jnp.float32)
    up_part = jnp.dot(full_rows, pieces[1], preferred_element_type=jnp.float32)
    hidden = (jax.nn.silu(gate) * up_part).astype(jnp.bfloat16)
    partial_out = jnp.dot(
        hidden,
        lax.all_gather(down_weight, "sp", axis=1, tiled=True),
        preferred_element_type=jnp.float32,
    )
    ffn = lax.psum_scatter(
        partial_out.astype(jnp.bfloat16), "tp", scatter_dimension=1, tiled=True
    ).astype(jnp.float32)
    return (stream + 0.5 * ffn).astype(jnp.bfloat16)


def flip(index, bits):
    bit = 1
    while bit <= bits:
        if (bits // bit) % 2:
            index = index + bit - 2 * bit * ((index // bit) % 2)
        bit *= 2
    return index


def nt_dot(a, b):
    return lax.dot_general(a, b, (((1,), (1,)), ((), ())), preferred_element_type=jnp.float32)


def dot(a, b):
    return jnp.dot(a, b, preferred_element_type=jnp.float32)


def layer_kernel(
    sp_count,
    widths,
    q1_ref,
    q2_ref,
    k1_ref,
    k2_ref,
    v_ref,
    lam_ref,
    residual_ref,
    gain_ref,
    proj_hbm,
    gate_ref,
    up_ref,
    down_ref,
    out_ref,
    k1b,
    k2b,
    vb,
    proj_ref,
    peak,
    total,
    acc,
    wg,
    wu,
    wd,
    mp,
    rsb,
    stream,
    act,
    gains,
    hid,
    c1,
    c1r,
    po,
    c2,
    c2r,
    c3,
    c3r,
    kv_ss,
    kv_rs,
    w_ss,
    w_rs,
    f_ss,
    f_rs,
    own_sem,
    g_ss,
    g_rs,
    rs_ss,
    rs_rs,
    az_ss,
    az_rs,
    ax_ss,
    ax_rs,
    ac_ss,
    ac_rs,
    c_ss,
    c_rs,
):
    s = lax.axis_index("sp")
    t = lax.axis_index("tp")
    y = lax.axis_index("grp")
    rows, blk = residual_ref.shape
    cols = wg.shape[2]
    hidden_all = gate_ref.shape[1]
    value_size = acc.shape[2]
    xpeer, cpeer, dpeer = flip(t, 2), flip(t, 1), flip(t, 3)
    others = range(1, sp_count)

    def remote(src, dst, ssem, rsem, **where):
        return pltpu.make_async_remote_copy(
            src_ref=src,
            dst_ref=dst,
            send_sem=ssem,
            recv_sem=rsem,
            device_id=where,
            device_id_type=pl.DeviceIdType.MESH,
        )

    barrier = pltpu.get_barrier_semaphore()
    for k in others:
        pl.semaphore_signal(barrier, inc=1, device_id={"sp": flip(s, k)}, device_id_type=pl.DeviceIdType.MESH)
        pl.semaphore_signal(barrier, inc=1, device_id={"tp": flip(t, k)}, device_id_type=pl.DeviceIdType.MESH)
    pl.semaphore_signal(barrier, inc=1, device_id={"grp": 1 - y}, device_id_type=pl.DeviceIdType.MESH)
    pl.semaphore_wait(barrier, 2 * (sp_count - 1) + 1)

    sends = []

    right, left = lax.rem(s + 1, sp_count), lax.rem(s + sp_count - 1, sp_count)
    has_right, has_left = s + 1 < sp_count, s > 0

    def kv_copy(back):
        pairs = ((k1_ref, k1b), (k2_ref, k2b), (v_ref, vb))
        return [
            remote(dst.at[back] if back else src, dst.at[back + 1], kv_ss.at[i, back], kv_rs.at[i, back + 1], sp=right)
            for i, (src, dst) in enumerate(pairs)
        ]

    kv_copies = {back: kv_copy(back) for back in range(sp_count - 1)}

    def kv_send(back):
        @pl.when(jnp.logical_and(has_right, s >= back))
        def _():
            for copy in kv_copies[back]:
                copy.start()

    kv_send(0)

    half_d = wg.shape[1] // 2
    half_c = cols // 2
    extra = sp_count * cols - hidden_all
    half_last = (cols - extra) // 2
    d_half = pl.ds(pl.multiple_of(y * half_d, half_d), half_d)
    last = sp_count - 1

    def w_copy(kind, k, source, target, short):
        src, dst = ((gate_ref, wg), (up_ref, wu), (down_ref, wd))[kind]
        begin = hidden_all - cols + extra if short else pl.multiple_of(target * cols, 128)
        skip, size = (extra, cols - extra) if short else (0, cols)
        if kind < 2:
            piece = src.at[d_half, pl.ds(begin, size)]
            place = dst.at[source, d_half, pl.ds(skip, size)]
        else:
            part = y * (size // 2)
            piece = src.at[pl.ds(pl.multiple_of(begin + part, 64), size // 2), :]
            place = dst.at[source, pl.ds(pl.multiple_of(skip + part, 64), size // 2)]
        return remote(piece, place, w_ss.at[kind, k], w_rs.at[kind, k], sp=flip(s, k)), place

    def f_copy(kind, k, short):
        _, place = w_copy(kind, k, flip(s, k), s, short)
        return remote(place, place, f_ss.at[kind, k], f_rs.at[kind, k], grp=1 - y)

    def either(test, action):
        pl.when(test)(lambda: action(True))
        pl.when(jnp.logical_not(test))(lambda: action(False))

    def send_weights(kinds, rightward):
        for k in others:

            def go(short, k=k):
                for kind in kinds:
                    w_copy(kind, k, s, flip(s, k), short)[0].start()

            target = flip(s, k)
            if rightward:
                pl.when(target == last)(functools.partial(go, True))
                pl.when(jnp.logical_and(target > s, target != last))(functools.partial(go, False))
            else:
                pl.when(target < s)(functools.partial(go, False))

    @pl.when(s == last)
    def _():
        wg[:, :, :extra] = jnp.zeros((sp_count, wg.shape[1], extra), jnp.bfloat16)
        wu[:, :, :extra] = jnp.zeros((sp_count, wg.shape[1], extra), jnp.bfloat16)
        wd[:, :extra, :] = jnp.zeros((sp_count, extra, blk), jnp.bfloat16)

    send_weights((0, 1), False)
    proj_copy = pltpu.make_async_copy(proj_hbm, proj_ref, own_sem.at[3])
    proj_copy.start()
    def own_copy(kind, short):
        src, dst = ((gate_ref, wg), (up_ref, wu), (down_ref, wd))[kind]
        begin = hidden_all - cols + extra if short else pl.multiple_of(s * cols, 128)
        skip, size = (extra, cols - extra) if short else (0, cols)
        if kind < 2:
            return pltpu.make_async_copy(src.at[:, pl.ds(begin, size)], dst.at[s, :, pl.ds(skip, size)], own_sem.at[kind])
        return pltpu.make_async_copy(src.at[pl.ds(begin, size), :], dst.at[s, pl.ds(skip, size)], own_sem.at[kind])

    def start_own(short):
        for kind in range(3):
            own_copy(kind, short).start()

    either(s == last, start_own)

    gains[t] = jnp.broadcast_to(gain_ref[...].reshape(1, blk), gains.shape[1:])
    gain_copies = []
    for k in others:
        copy = remote(gains.at[t], gains.at[t], g_ss.at[k], g_rs.at[k], tp=flip(t, k))
        copy.start()
        gain_copies.append(copy)
        sends.append(copy)

    q_refs = (q1_ref, q2_ref)
    lane = lax.broadcasted_iota(jnp.int32, (1, 2 * widths[0]), 1)

    def block(keys, v, diagonal):
        for group in range(2):
            width = widths[group]
            values = v[:, group, :]
            for m in range(2):
                if width % 128:
                    span = slice(0, 2 * width)
                    queries = q_refs[group][:, span]
                    queries = jnp.where(lane // width == m, queries.astype(jnp.float32), 0.0).astype(jnp.bfloat16)
                else:
                    span = slice(m * width, (m + 1) * width)
                    queries = q_refs[group][:, span]
                scores = nt_dot(queries, keys[group][:, span]) * width ** (-0.5)
                state = 2 * group + m
                if diagonal:
                    allowed = lax.broadcasted_iota(jnp.int32, (rows, rows), 1) <= lax.broadcasted_iota(
                        jnp.int32, (rows, rows), 0
                    )
                    scores = jnp.where(allowed, scores, -1e30)
                    top = jnp.max(scores, axis=1, keepdims=True)
                    weights = jnp.exp(scores - top)
                    peak[state] = top
                    total[state] = jnp.sum(weights, axis=1, keepdims=True)
                    acc[state] = dot(weights.astype(jnp.bfloat16), values)
                else:
                    before = peak[state]
                    top = jnp.maximum(before, jnp.max(scores, axis=1, keepdims=True))
                    fade = jnp.exp(before - top)
                    weights = jnp.exp(scores - top)
                    peak[state] = top
                    total[state] = total[state] * fade + jnp.sum(weights, axis=1, keepdims=True)
                    acc[state] = acc[state] * fade + dot(weights.astype(jnp.bfloat16), values)

    block((k1_ref, k2_ref), v_ref, True)
    for back in others:

        @pl.when(s >= back)
        def _(back=back):
            for copy in kv_copies[back - 1]:
                copy.wait_recv()

        if back in kv_copies:
            kv_send(back)
    send_weights((0, 1), True)
    for back in others:

        @pl.when(s >= back)
        def _(back=back):
            block((k1b.at[back], k2b.at[back]), vb.at[back], False)

    proj_copy.wait()
    attended = []
    for group in range(2):
        first = acc[2 * group] / total[2 * group]
        second = acc[2 * group + 1] / total[2 * group + 1]
        differ = first - lam_ref[0, group] * second
        scale = lax.rsqrt(jnp.mean(differ * differ, axis=1, keepdims=True) + 1e-06)
        attended.append((0.8 * differ * scale).astype(jnp.bfloat16))

    def project(owner):
        columns = pl.ds(pl.multiple_of(owner * blk, blk), blk)
        return dot(attended[0], proj_ref[0, :, columns]) + dot(attended[1], proj_ref[1, :, columns])

    rs_copies = {}
    for k in (2, 3, 1):
        mp[k] = project(flip(t, k)).astype(jnp.bfloat16)
        rs_copies[k] = remote(mp.at[k], rsb.at[k], rs_ss.at[k], rs_rs.at[k], tp=flip(t, k))
        rs_copies[k].start()
        sends.append(rs_copies[k])
    mixed = project(t)
    for k in (1, 2, 3):
        rs_copies[k].wait_recv()
        mixed = mixed + rsb[k].astype(jnp.float32)
    stream[...] = residual_ref[...].astype(jnp.float32) + mixed
    act[t, s] = stream[...].astype(jnp.bfloat16)

    ax, ac0, ac1 = {}, {}, {}
    for k in range(sp_count):
        row = flip(s, k)
        ax[k] = remote(act.at[t, row], act.at[t, row], ax_ss.at[k], ax_rs.at[k], tp=xpeer)
        ac0[k] = remote(act.at[t, row], act.at[t, row], ac_ss.at[0, k], ac_rs.at[0, k], tp=cpeer)
        ac1[k] = remote(act.at[xpeer, row], act.at[xpeer, row], ac_ss.at[1, k], ac_rs.at[1, k], tp=cpeer)

    def along_line(k, action):
        row = flip(s, k)
        piece = act.at[t, row]

        @pl.when(jnp.logical_and(has_right, row <= s))
        def _():
            action(remote(piece, piece, az_ss.at[0, row], az_rs.at[row], sp=right))

        @pl.when(jnp.logical_and(has_left, row >= s))
        def _():
            action(remote(piece, piece, az_ss.at[1, row], az_rs.at[row], sp=left))

    along_line(0, lambda copy: copy.start())
    send_weights((2,), True)
    send_weights((2,), False)

    def pass_on(k):
        if k:
            row = flip(s, k)
            piece = act.at[t, row]
            remote(piece, piece, az_ss.at[0, row], az_rs.at[row], sp=right).wait_recv()
            along_line(k, lambda copy: copy.start())
        ax[k].start()
        ac0[k].start()

    def pass_inside(k):
        ax[k].wait_recv()
        ac1[k].start()

    def hand_over(kinds, k):
        def go(short):
            for kind in kinds:
                w_copy(kind, k, flip(s, k), s, short)[0].wait_recv()
                f_copy(kind, k, short).start()

        either(s == last, go)

    def await_weights(kinds):
        def go(short):
            for kind in kinds:
                own_copy(kind, short).wait()
                for k in others:
                    f_copy(kind, k, short).wait_recv()

        either(s == last, go)

    turns = (0, 1, 3, 2)
    pass_on(0)
    for at, k in enumerate(turns[1:]):
        hand_over((0, 1), at + 1)
        pass_on(k)
        pass_inside(turns[at])
    pass_inside(turns[-1])

    for copy in gain_copies:
        copy.wait_recv()
    await_weights((0, 1))
    column = jnp.minimum(s * cols, hidden_all - cols) + lax.broadcasted_iota(jnp.int32, (1, cols), 1)
    mine = column >= s * cols

    def hidden_of(k):
        row = flip(s, k)
        ac0[k].wait_recv()
        ac1[k].wait_recv()
        squares = jnp.zeros((rows, 1), jnp.float32)
        for part in range(sp_count):
            piece = act[part, row].astype(jnp.float32)
            squares = squares + jnp.sum(piece * piece, axis=1, keepdims=True)
        scale = lax.rsqrt(squares / (sp_count * blk) + 1e-06)
        gate = jnp.zeros((rows, cols), jnp.float32)
        up = jnp.zeros((rows, cols), jnp.float32)
        for part in range(sp_count):
            gain = gains[part, 0:1, :].astype(jnp.float32)
            normed = (act[part, row].astype(jnp.float32) * scale * gain).astype(jnp.bfloat16)
            gate = gate + dot(normed, wg[part])
            up = up + dot(normed, wu[part])
        hidden = gate / (1.0 + jnp.exp(-gate)) * up
        hid[k] = jnp.where(mine, hidden, 0.0).astype(jnp.bfloat16)

    r1, r2, r3 = {}, {}, {}
    for k in range(sp_count):
        r1[k] = remote(c1.at[k], c1r.at[k], c_ss.at[0, k], c_rs.at[0, k], tp=cpeer)
        r2[k] = remote(c2.at[k], c2r.at[k], c_ss.at[1, k], c_rs.at[1, k], tp=xpeer)
        if k:
            r3[k] = remote(c3.at[k], c3r.at[k], c_ss.at[2, k], c_rs.at[2, k], sp=flip(s, k))

    def down_of(k):
        hidden = hid[k]
        c1[k, 0] = dot(hidden, wd[cpeer]).astype(jnp.bfloat16)
        c1[k, 1] = dot(hidden, wd[dpeer]).astype(jnp.bfloat16)
        r1[k].start()
        po[k, 1] = dot(hidden, wd[xpeer])
        po[k, 0] = dot(hidden, wd[t])

    def across(k):
        r1[k].wait_recv()
        c2[k] = (po[k, 1] + c1r[k, 1].astype(jnp.float32)).astype(jnp.bfloat16)
        r2[k].start()

    def along(k):
        r2[k].wait_recv()
        result = po[k, 0] + c1r[k, 0].astype(jnp.float32) + c2r[k].astype(jnp.float32)
        if k:
            c3[k] = result.astype(jnp.bfloat16)
            r3[k].start()
        else:
            po[0, 0] = result

    for at, k in enumerate(turns):
        hidden_of(k)
        if at + 1 < sp_count:
            hand_over((2,), at + 1)
    await_weights((2,))
    order = (3, 2, 1, 0)
    for at, k in enumerate(order):
        down_of(k)
        if at >= 1:
            across(order[at - 1])
        if at >= 2:
            along(order[at - 2])
    across(order[-1])
    along(order[-2])
    along(order[-1])

    ffn = po[0, 0]
    for k in order[:-1]:
        r3[k].wait_recv()
        ffn = ffn + c3r[k].astype(jnp.float32)
    out_ref[...] = (stream[...] + 0.5 * ffn).astype(jnp.bfloat16)

    for back in kv_copies:

        @pl.when(jnp.logical_and(has_right, s >= back))
        def _(back=back):
            for copy in kv_copies[back]:
                copy.wait_send()

    def finish():
        for k in others:

            def go(short, k=k):
                for kind in range(3):
                    w_copy(kind, k, s, flip(s, k), short)[0].wait_send()

            either(flip(s, k) == last, go)

        def gone(short):
            for k in others:
                for kind in range(3):
                    f_copy(kind, k, short).wait_send()

        either(s == last, gone)

    finish()
    for k in range(sp_count):
        along_line(k, lambda copy: copy.wait_send())
    for copies in (ax, ac0, ac1, r1, r2, r3):
        sends.extend(copies.values())
    for copy in sends:
        copy.wait_send()


def fits(axes, query_first, values, lambdas, residual, gate_weight):
    sp, tp = axes["sp"], axes["tp"]
    rows, blk = residual.shape
    depth, hidden_all = gate_weight.shape
    if axes["grp"] != 2 or sp != tp or tp != 4 or lambdas.shape[1] != 1:
        return False
    if depth != blk or blk % 128 or hidden_all % 128 or rows % 16:
        return False
    if (2 * query_first.shape[1]) % 256 or values.shape[2] % 128:
        return False
    cols = -(-hidden_all // (128 * sp)) * 128
    if cols * sp - hidden_all >= cols or cols > hidden_all:
        return False
    if (cols * sp - hidden_all) % 128 or blk % 32:
        return False
    need = 6 * sp * blk * cols + rows * blk * 2 * 20 * sp
    return need < 40 * 1024 * 1024


def one_device(
    axes,
    query_first,
    key_first,
    query_second,
    key_second,
    values,
    lambdas,
    residual,
    norm_gain,
    out_weight,
    gate_weight,
    up_weight,
    down_weight,
):
    if not fits(axes, query_first, values, lambdas, residual, gate_weight):
        return per_device(
            query_first,
            key_first,
            query_second,
            key_second,
            values,
            lambdas,
            residual,
            norm_gain,
            out_weight,
            gate_weight,
            up_weight,
            down_weight,
        )
    n = axes["sp"]
    rows, blk = residual.shape
    hidden_all = gate_weight.shape[1]
    cols = -(-hidden_all // (128 * n)) * 128
    value_size = values.shape[2]
    widths = (query_first.shape[1] // 2, query_second.shape[1] // 2)
    bf16, f32 = jnp.bfloat16, jnp.float32
    vmem = pl.BlockSpec(memory_space=pltpu.VMEM)
    smem = pl.BlockSpec(memory_space=pltpu.SMEM)
    hbm = pl.BlockSpec(memory_space=pl.ANY)
    dma = pltpu.SemaphoreType.DMA
    return pl.pallas_call(
        functools.partial(layer_kernel, n, widths),
        out_shape=jax.ShapeDtypeStruct((rows, blk), bf16),
        in_specs=[vmem] * 5 + [smem, vmem, vmem] + [hbm] * 4,
        out_specs=vmem,
        scratch_shapes=[
            pltpu.VMEM((n,) + key_first.shape, bf16),
            pltpu.VMEM((n,) + key_second.shape, bf16),
            pltpu.VMEM((n,) + values.shape, bf16),
            pltpu.VMEM(out_weight.shape, bf16),
            pltpu.VMEM((4, rows, 1), f32),
            pltpu.VMEM((4, rows, 1), f32),
            pltpu.VMEM((4, rows, value_size), f32),
            pltpu.VMEM((n, blk, cols), bf16),
            pltpu.VMEM((n, blk, cols), bf16),
            pltpu.VMEM((n, cols, blk), bf16),
            pltpu.VMEM((n, rows, blk), bf16),
            pltpu.VMEM((n, rows, blk), bf16),
            pltpu.VMEM((rows, blk), f32),
            pltpu.VMEM((n, n, rows, blk), bf16),
            pltpu.VMEM((n, 16, blk), bf16),
            pltpu.VMEM((n, rows, cols), bf16),
            pltpu.VMEM((n, 2, rows, blk), bf16),
            pltpu.VMEM((n, 2, rows, blk), bf16),
            pltpu.VMEM((n, 2, rows, blk), f32),
            pltpu.VMEM((n, rows, blk), bf16),
            pltpu.VMEM((n, rows, blk), bf16),
            pltpu.VMEM((n, rows, blk), bf16),
            pltpu.VMEM((n, rows, blk), bf16),
            dma((3, n)),
            dma((3, n)),
            dma((3, n)),
            dma((3, n)),
            dma((3, n)),
            dma((3, n)),
            dma((4,)),
            dma((n,)),
            dma((n,)),
            dma((n,)),
            dma((n,)),
            dma((2, n)),
            dma((n,)),
            dma((n,)),
            dma((n,)),
            dma((2, n)),
            dma((2, n)),
            dma((3, n)),
            dma((3, n)),
        ],
        compiler_params=pltpu.CompilerParams(
            collective_id=0, has_side_effects=True, vmem_limit_bytes=60 * 1024 * 1024
        ),
    )(
        query_first,
        query_second,
        key_first,
        key_second,
        values,
        lambdas.T,
        residual,
        norm_gain,
        out_weight,
        gate_weight,
        up_weight,
        down_weight,
    )

def solution(mesh):
    return jax.shard_map(
        functools.partial(one_device, dict(mesh.shape)),
        mesh=mesh,
        in_specs=(
            P(("grp", "sp"), "tp"),
            P(("grp", "sp"), "tp"),
            P(("grp", "sp"), "tp"),
            P(("grp", "sp"), "tp"),
            P(("grp", "sp"), None, "tp"),
            P(None, "tp"),
            P(("grp", "sp"), "tp"),
            P("tp"),
            P(None, "tp", None),
            P("sp", "tp"),
            P("sp", "tp"),
            P("tp", "sp"),
        ),
        out_specs=P(("grp", "sp"), "tp"),
        check_vma=False,
    )
```
